32 devices in a mesh: sp: 8 (over z, x), dp: 4 (over y, core).
Axes of the slice: x: 2, y: 2, z: 4, core: 2. Of those that a mesh axis runs over, the one named last changes fastest.
Arguments:
- hidden_in: bfloat16 [4, 1024, 2048], P('dp', 'sp'), may hold values from -6 to 6
- mix_cotangent: bfloat16 [4, 1024, 4096], P('dp', 'sp'), may hold values from -0.119628906 to 0.119628906
- query_weight: bfloat16 [2048, 4096], P('dp', 'sp'), may hold values from -0.125 to 0.125
- key_weight: bfloat16 [2048, 4096], P('dp', 'sp'), may hold values from -0.125 to 0.125
- value_weight: bfloat16 [2048, 4096], P('dp', 'sp'), may hold values from -0.125 to 0.125
- decay_log: float32 [16], P('sp'), may hold values from -0.034 to -0.00029296875, as said below
Outputs:
- grad_hidden: bfloat16 [4, 1024, 2048], P('dp', 'sp')
- grad_query: float32 [2048, 4096], P('dp', 'sp')
- grad_key: float32 [2048, 4096], P('dp', 'sp')
- grad_value: float32 [2048, 4096], P('dp', 'sp')
The draws below stay inside these ranges and needn't reach their ends.
Inputs may be any that keep to these rules, and one draw needn't show every extreme that they name: Each head's decay_log is negative.
All inputs are finite; a program needn't handle non-finite values.
Results may differ from the reference program's by a relative error of at most 0.015.
Values may be sent and summed in bfloat16 or wider, within the bound.
A program may use at most 64 MiB of HBM per device.

```python
import jax
import jax.numpy as jnp
from jax import lax

D = 2048
HEADS = 16
BLOCK = 128
WIDTH = 4096
SEQ_LEN = 1024
SEQS = 4
N_SP = 8


def draw_decay_log(key, part):
    key_fast = jax.random.fold_in(key, 11)
    key_quick = jax.random.fold_in(key, 12)
    key_slow = jax.random.fold_in(key, 13)
    fast = jax.random.bernoulli(key_fast, 0.5, (HEADS,))
    quick_rate = jax.random.uniform(key_quick, (HEADS,), jnp.float32, 0.01, 0.034)
    slow_rate = jax.random.uniform(key_slow, (HEADS,), jnp.float32, 0.3, 2.0) / SEQ_LEN
    return -jnp.where(fast, quick_rate, slow_rate).astype(jnp.float32)


def block_levels(own_key, extent, cuts, smallest, largest):
    gain = 1.0
    for position, parts in cuts:
        heights = jax.random.uniform(jax.random.fold_in(jax.random.fold_in(own_key, 6), position), (parts,), jnp.float32, smallest / len(cuts), largest / len(cuts))
        gain = gain * jnp.repeat(jnp.exp(heights), extent[position] // parts).reshape((-1,) + (1,) * (len(extent) - 1 - position))
    return gain


def noise(rng, extent, scale, reach, split=(), kind=jnp.bfloat16):
    array = scale * jax.random.normal(rng, extent, jnp.float32)
    if split:
        array = array * block_levels(rng, extent, split, -0.22, 0.18)
    return jnp.clip(array, -reach, reach).astype(kind)


def setup_inputs(seed: int = 0) -> dict:
    seeds = jax.random.split(jax.random.key(seed), 7)
    return {
        "hidden_in": noise(seeds[0], (SEQS, SEQ_LEN, D), 1.0, 6.0, ((0, 4), (1, 8))),
        "mix_cotangent": noise(seeds[1], (SEQS, SEQ_LEN, WIDTH), 0.02, 0.119628906, ((0, 4), (1, 8))),
        "query_weight": noise(seeds[2], (D, WIDTH), D ** -0.5, 0.125, ((0, 4), (1, 8))),
        "key_weight": noise(seeds[3], (D, WIDTH), D ** -0.5, 0.125, ((0, 4), (1, 8))),
        "value_weight": noise(seeds[4], (D, WIDTH), D ** -0.5, 0.125, ((0, 4), (1, 8))),
        "decay_log": draw_decay_log(jax.random.fold_in(seeds[6], 71), 0),
    }


def head_grads(queries, key_rows, values, cotangent, log_rate):
    length = queries.shape[0]
    head_dim = queries.shape[1]
    blocks = length // BLOCK
    scale = head_dim ** -0.5
    keys_scaled = (key_rows.astype(jnp.float32) * scale).astype(jnp.bfloat16)
    offsets = jnp.arange(BLOCK, dtype=jnp.float32)
    spread = offsets[:, None] - offsets[None, :]
    inner_decay = jnp.where(spread >= 0, jnp.exp(log_rate * jnp.maximum(spread, 0.0)), 0.0)
    query_decay = jnp.exp(log_rate * (offsets + 1.0))
    key_decay = jnp.exp(log_rate * (BLOCK - 1.0 - offsets))
    block_decay = jnp.exp(log_rate * BLOCK)

    def split_blocks(series):
        return series.reshape(blocks, BLOCK, series.shape[-1])

    def forward(carried, inputs):
        query_block, key_block, value_block, grad_block = inputs
        mixed = (jnp.dot(grad_block, value_block.T, preferred_element_type=jnp.float32) * inner_decay).astype(jnp.bfloat16)
        within = jnp.dot(mixed, key_block, preferred_element_type=jnp.float32)
        across = jnp.dot(grad_block, carried.astype(jnp.bfloat16).T, preferred_element_type=jnp.float32) * query_decay[:, None]
        weighted = (key_block.astype(jnp.float32) * key_decay[:, None]).astype(jnp.bfloat16)
        updated = carried * block_decay + jnp.dot(weighted.T, value_block, preferred_element_type=jnp.float32)
        return updated, (within + across, mixed)

    def backward(carried, inputs):
        query_block, key_block, value_block, grad_block, mixed = inputs
        scores = (jnp.dot(query_block, key_block.T, preferred_element_type=jnp.float32) * inner_decay).astype(jnp.bfloat16)
        state_bf = carried.astype(jnp.bfloat16)
        grad_v = jnp.dot(scores.T, grad_block, preferred_element_type=jnp.float32) + jnp.dot(key_block, state_bf, preferred_element_type=jnp.float32) * key_decay[:, None]
        grad_k = (jnp.dot(mixed.T, query_block, preferred_element_type=jnp.float32) + jnp.dot(value_block, state_bf.T, preferred_element_type=jnp.float32) * key_decay[:, None]) * scale
        weighted = (query_block.astype(jnp.float32) * query_decay[:, None]).astype(jnp.bfloat16)
        updated = carried * block_decay + jnp.dot(weighted.T, grad_block, preferred_element_type=jnp.float32)
        return updated, (grad_k, grad_v)

    inputs = (split_blocks(queries), split_blocks(keys_scaled), split_blocks(values), split_blocks(cotangent))
    initial = jnp.zeros((head_dim, values.shape[-1]), jnp.float32)
    final_state, (grad_q, mixed_all) = lax.scan(forward, initial, inputs)
    final_back, (grad_k, grad_v) = lax.scan(backward, initial, inputs + (mixed_all,), reverse=True)
    return grad_q.reshape(length, -1), grad_k.reshape(length, -1), grad_v.reshape(length, -1)


def group_grads(log_rates, queries, key_rows, values, cotangent):
    length = queries.shape[0]
    head_count = log_rates.shape[0]

    def by_head(series):
        return series.reshape(length, head_count, -1).transpose(1, 0, 2)

    def to_rows(series):
        return series.transpose(1, 0, 2).reshape(length, -1)

    grad_q, grad_k, grad_v = jax.vmap(head_grads)(by_head(queries), by_head(key_rows), by_head(values), by_head(cotangent), log_rates)
    return jnp.concatenate((to_rows(grad_q), to_rows(grad_k), to_rows(grad_v)), axis=1).astype(jnp.bfloat16)


def reference(hidden_in, mix_cotangent, query_weight, key_weight, value_weight, decay_log):
    weights = jnp.concatenate((query_weight, key_weight, value_weight), axis=1)
    all_width = query_weight.shape[1]
    model_width = query_weight.shape[0]

    def one_sequence(seq_pair):
        seq_rows, seq_cotangent = seq_pair
        projected = jnp.dot(seq_rows, weights, preferred_element_type=jnp.float32).astype(jnp.bfloat16)
        gradients = group_grads(decay_log, projected[:, :all_width], projected[:, all_width:2 * all_width], projected[:, 2 * all_width:], seq_cotangent)
        length = seq_rows.shape[0]
        split_grads = gradients.reshape(length, 3, N_SP, -1).astype(jnp.float32)
        split_weights = weights.reshape(model_width, 3, N_SP, -1).astype(jnp.float32)
        partials = jnp.einsum('ltgc,dtgc->gld', split_grads, split_weights)
        rounded = lax.optimization_barrier(partials.astype(jnp.bfloat16)).astype(jnp.float32)
        return jnp.sum(rounded, axis=0).astype(jnp.bfloat16), gradients

    grad_hidden, all_grads = lax.map(one_sequence, (hidden_in, mix_cotangent))
    flat_rows = hidden_in.reshape(-1, model_width)
    flat_grads = all_grads.reshape(-1, 3 * all_width)
    summed = lax.dot_general(flat_rows, flat_grads, (((0,), (0,)), ((), ())), preferred_element_type=jnp.float32) / SEQS
    return grad_hidden, summed[:, :all_width], summed[:, all_width:2 * all_width], summed[:, 2 * all_width:]
```

```python
import functools

import jax
import jax.numpy as jnp
from jax import lax
from jax.experimental import pallas as pl
from jax.experimental.pallas import tpu as pltpu
from jax.sharding import PartitionSpec as P

BLOCK = 128
SUBS = 2
F32 = jnp.float32
BF16 = jnp.bfloat16
MESH = pl.DeviceIdType.MESH
NT = (((1,), (1,)), ((), ()))
TN = (((0,), (0,)), ((), ()))
VMEM_LIMIT = 60 * 1024 * 1024


def dot(a, b, dims=(((1,), (0,)), ((), ()))):
    return lax.dot_general(a, b, dims, preferred_element_type=F32)


def remote(src, dst, send, recv, where):
    return pltpu.make_async_remote_copy(
        src_ref=src, dst_ref=dst, send_sem=send, recv_sem=recv, device_id=where, device_id_type=MESH
    )


def greet(targets):
    barrier = pltpu.get_barrier_semaphore()
    for where in targets:
        pl.semaphore_signal(barrier, inc=1, device_id=where, device_id_type=MESH)
    pl.semaphore_wait(barrier, len(targets))


def gather_kernel(
    n, m, h_in, c_in, wq, wk, wv, h_all, c_all, w_all,
    h_recv, h_line, h_side, c_send, c_recv, w_far, w_near, w_recv,
):
    s = lax.axis_index("sp")
    d = lax.axis_index("dp")
    z, x = s // 2, s % 2
    y, core = d // 2, d % 2
    nz, ny = n // 2, m // 2
    rows = h_in.shape[0]
    sub_rows = rows // SUBS
    depth, columns = wq.shape
    side = s + 1 - 2 * x
    mate = d + 1 - 2 * core

    def far(o):
        return ((y + o) % ny) * 2 + core

    greet(
        [{"sp": (s + k) % n} for k in range(1, n)]
        + [{"dp": mate}]
        + [{"dp": far(o)} for o in range(1, ny)]
    )

    def h_copy(src_z, src_x, sub, dest, send, own=False):
        block = src_z * 2 + src_x
        place = pl.ds(pl.multiple_of(block * rows + sub * sub_rows, sub_rows), sub_rows)
        src = h_in.at[pl.ds(sub * sub_rows, sub_rows)] if own else h_all.at[place]
        return remote(src, h_all.at[place], send, h_recv.at[block, sub], {"sp": dest})

    def w_copy(src_d, j, dest, send, own=False):
        place = w_all.at[
            pl.ds(pl.multiple_of(src_d * depth, depth), depth), pl.ds(j * columns, columns)
        ]
        return remote((wq, wk, wv)[j] if own else place, place, send, w_recv.at[src_d, j], {"dp": dest})

    def c_copy(k):
        to = (s + k) % n
        return remote(
            c_in.at[:, pl.ds(pl.multiple_of(to * columns, columns), columns)],
            c_all.at[pl.ds(pl.multiple_of(s * rows, rows), rows)],
            c_send.at[k - 1],
            c_recv.at[k - 1],
            {"sp": to},
        )

    def line(k, sub, up, own):
        source = (z - k) if up else (z + k)
        dest = (s + 2) if up else (s - 2)
        return h_copy(source, x, sub, dest, h_line.at[k, sub, int(up)], own)

    def goes(k, up):
        if up:
            return jnp.logical_and(z - k >= 0, z + 1 < nz)
        return jnp.logical_and(z + k < nz, z >= 1)

    def arrives(k, up):
        return (z - k >= 0) if up else (z + k < nz)

    for sub in range(SUBS):
        for up in (True, False):

            @pl.when(goes(0, up))
            def _():
                line(0, sub, up, True).start()

        h_copy(z, x, sub, side, h_side.at[0, sub, 0], True).start()
    for j in range(3):
        for o in range(1, ny):
            w_copy(d, j, far(o), w_far.at[o, j], True).start()
        w_copy(d, j, mate, w_near.at[0, j], True).start()
    for k in range(1, n):
        c_copy(k).start()

    h_all[pl.ds(pl.multiple_of(s * rows, rows), rows), :] = h_in[...]
    c_all[pl.ds(pl.multiple_of(s * rows, rows), rows), :] = c_in[
        :, pl.ds(pl.multiple_of(s * columns, columns), columns)
    ]
    for j, w in enumerate((wq, wk, wv)):
        w_all[pl.ds(pl.multiple_of(d * depth, depth), depth), j * columns : (j + 1) * columns] = w[...]

    def pass_weights(j):
        for o in range(1, ny):
            w_copy(far(o), j, mate, w_near.at[o, j]).wait_recv()
            w_copy(far(o), j, mate, w_near.at[o, j]).start()

    passed = 0
    for k in range(1, nz):
        for sub in range(SUBS):
            for up in (True, False):

                @pl.when(arrives(k, up))
                def _():
                    source = (z - k) if up else (z + k)
                    h_copy(source, x, sub, side, h_side.at[k, sub, int(up)]).wait_recv()
                    h_copy(source, x, sub, side, h_side.at[k, sub, int(up)]).start()

                @pl.when(goes(k, up))
                def _():
                    line(k, sub, up, False).start()

        if passed < 3:
            pass_weights(passed)
            passed += 1
    for j in range(passed, 3):
        pass_weights(j)

    for j in range(3):
        w_copy(mate, j, mate, w_near.at[0, j]).wait_recv()
        for o in range(1, ny):
            other = far(o) + 1 - 2 * core
            w_copy(other, j, mate, w_near.at[o, j]).wait_recv()
    for zz in range(nz):
        for sub in range(SUBS):
            h_copy(zz, 1 - x, sub, side, h_side.at[0, sub, 0]).wait_recv()
    for k in range(1, n):
        c_copy(k).wait_recv()
    for k in range(1, n):
        c_copy(k).wait_send()
    for j in range(3):
        for o in range(ny):
            w_copy(d, j, mate, w_near.at[o, j]).wait_send()
            if o:
                w_copy(d, j, far(o), w_far.at[o, j]).wait_send()
    for sub in range(SUBS):
        h_copy(z, x, sub, side, h_side.at[0, sub, 0]).wait_send()
        for up in (True, False):
            for k in range(nz):

                @pl.when(goes(k, up))
                def _():
                    line(k, sub, up, False).wait_send()

                if k:

                    @pl.when(arrives(k, up))
                    def _():
                        h_copy(z, x, sub, side, h_side.at[k, sub, int(up)]).wait_send()


def gather(n, m, h, c, wq, wk, wv):
    rows, width = h.shape
    depth, columns = wq.shape
    vmem = pl.BlockSpec(memory_space=pltpu.VMEM)
    dma = pltpu.SemaphoreType.DMA
    return pl.pallas_call(
        functools.partial(gather_kernel, n, m),
        out_shape=(
            jax.ShapeDtypeStruct((rows * n, width), BF16),
            jax.ShapeDtypeStruct((rows * n, columns), BF16),
            jax.ShapeDtypeStruct((depth * m, 3 * columns), BF16),
        ),
        in_specs=[vmem] * 5,
        out_specs=(vmem,) * 3,
        scratch_shapes=[
            dma((n, SUBS)),
            dma((n // 2, SUBS, 2)),
            dma((n // 2, SUBS, 2)),
            dma((n - 1,)),
            dma((n - 1,)),
            dma((m // 2, 3)),
            dma((m // 2, 3)),
            dma((m, 3)),
        ],
        compiler_params=pltpu.CompilerParams(
            collective_id=0, has_side_effects=True, vmem_limit_bytes=VMEM_LIMIT
        ),
        name="gather_all",
    )(h, c, wq, wk, wv)


def mixer_kernel(heads, rate, h_all, c_all, w_all, g_all, p_all, state, back):
    length = h_all.shape[0]
    columns = c_all.shape[1]
    dim = columns // heads
    blocks = length // BLOCK
    scale = dim ** (-0.5)
    step = 2 * BLOCK if length % (2 * BLOCK) == 0 else BLOCK

    @pl.loop(0, length // step)
    def _(i):
        at = pl.ds(pl.multiple_of(i * step, step), step)
        for j in range(3):
            value = dot(h_all[at, :], w_all[:, j * columns : (j + 1) * columns]).astype(BF16)
            if j == 1:
                value = (value.astype(F32) * scale).astype(BF16)
            p_all[at, j * columns : (j + 1) * columns] = value

    row = lax.broadcasted_iota(jnp.int32, (BLOCK, BLOCK), 0).astype(F32)
    col = lax.broadcasted_iota(jnp.int32, (BLOCK, BLOCK), 1).astype(F32)
    place = lax.broadcasted_iota(jnp.int32, (BLOCK, dim), 0).astype(F32)
    spread = row - col
    state[...] = jnp.zeros_like(state)
    back[...] = jnp.zeros_like(back)

    @pl.loop(0, blocks)
    def _(i):
        for h in range(heads):
            g = rate[h]
            inner = jnp.where(spread >= 0, jnp.exp(g * jnp.maximum(spread, 0.0)), 0.0)
            inner_t = jnp.where(spread <= 0, jnp.exp(g * jnp.maximum(-spread, 0.0)), 0.0)
            query_decay = jnp.exp(g * (place + 1.0))
            key_decay = jnp.exp(g * (BLOCK - 1.0 - place))
            block_decay = jnp.exp(jnp.full((1, dim), g * BLOCK, F32))
            parts = [slice(j * columns + h * dim, j * columns + (h + 1) * dim) for j in range(3)]

            at = pl.ds(pl.multiple_of(i * BLOCK, BLOCK), BLOCK)
            k, v = p_all[at, parts[1]], p_all[at, parts[2]]
            c = c_all[at, parts[0]]
            mixed = (dot(c, v, NT) * inner).astype(BF16)
            held = state[h]
            grad_q = dot(mixed, k) + dot(c, held.astype(BF16), NT) * query_decay
            weighted = (k.astype(F32) * key_decay).astype(BF16)
            state[h] = held * block_decay + dot(weighted, v, TN)
            g_all[at, parts[0]] = grad_q.astype(BF16)

            at = pl.ds(pl.multiple_of((blocks - 1 - i) * BLOCK, BLOCK), BLOCK)
            q, k, v = (p_all[at, part] for part in parts)
            c = c_all[at, parts[0]]
            mixed_t = (dot(v, c, NT) * inner_t).astype(BF16)
            scores_t = (dot(k, q, NT) * inner_t).astype(BF16)
            held = back[h]
            held_bf = held.astype(BF16)
            grad_v = dot(scores_t, c) + dot(k, held_bf) * key_decay
            grad_k = (dot(mixed_t, q) + dot(v, held_bf, NT) * key_decay) * scale
            weighted = (q.astype(F32) * query_decay).astype(BF16)
            back[h] = held * block_decay + dot(weighted, c, TN)
            g_all[at, parts[1]] = grad_k.astype(BF16)
            g_all[at, parts[2]] = grad_v.astype(BF16)


def mixer(rate, h_all, c_all, w_all):
    heads = rate.shape[0]
    length = h_all.shape[0]
    width = w_all.shape[1]
    dim = c_all.shape[1] // heads
    vmem = pl.BlockSpec(memory_space=pltpu.VMEM)
    return pl.pallas_call(
        functools.partial(mixer_kernel, heads),
        out_shape=jax.ShapeDtypeStruct((length, width), BF16),
        in_specs=[pl.BlockSpec(memory_space=pltpu.SMEM), vmem, vmem, vmem],
        out_specs=vmem,
        scratch_shapes=[
            pltpu.VMEM((length, width), BF16),
            pltpu.VMEM((heads, dim, dim), F32),
            pltpu.VMEM((heads, dim, dim), F32),
        ],
        compiler_params=pltpu.CompilerParams(vmem_limit_bytes=VMEM_LIMIT),
        name="mixer",
    )(rate, h_all, c_all, w_all)


def scatter_kernel(
    n, m, h_all, w_all, g_all, dh, dq, dk, dv,
    part, ring, turned, near_out, near_in, far_out, far_in,
    r_send, r_recv, n_send, n_recv, f_send, f_recv,
):
    s = lax.axis_index("sp")
    d = lax.axis_index("dp")
    z, x = s // 2, s % 2
    y, core = d // 2, d % 2
    nz, ny = n // 2, m // 2
    rows, width = dh.shape
    depth, columns = dq.shape
    half = rows // 2
    sub_rows = half // SUBS
    mate = d + 1 - 2 * core
    me = x * (n - 1 - z) + (1 - x) * z

    def at_ring(p):
        p = (p + 2 * n) % n
        hi = p // nz
        return (hi * (n - 1 - p) + (1 - hi) * p) * 2 + hi

    def far(o):
        return ((y + o) % ny) * 2 + core

    right, left = at_ring(me + 1), at_ring(me - 1)
    greet(
        [{"sp": right}, {"sp": left}, {"dp": mate}] + [{"dp": far(o)} for o in range(1, ny)]
    )

    def own(offset):
        return pl.multiple_of(at_ring(me + offset) * rows, rows)

    ready = set()

    def compute(offset):
        offset = offset % n
        if offset in ready:
            return
        ready.add(offset)
        base = own(offset)
        chunk = width // 4

        @pl.loop(0, 4)
        def _(i):
            at = pl.ds(pl.multiple_of(i * chunk, chunk), chunk)
            part[pl.ds(base, rows), at] = dot(g_all[pl.ds(base, rows), :], w_all[at, :], NT).astype(BF16)

    def r_copy(step, way, sub):
        lane = (slice(0, half), slice(half, rows))[way].start + sub * sub_rows
        if step == 0:
            base = own(-1 if way == 0 else 1)
            src = part.at[pl.ds(pl.multiple_of(base + lane, sub_rows), sub_rows)]
        else:
            src = ring.at[step - 1, way, sub]
        return remote(
            src,
            ring.at[step, way, sub],
            r_send.at[step, way, sub],
            r_recv.at[step, way, sub],
            {"sp": right if way == 0 else left},
        )

    def process(step):
        for sub in range(SUBS):
            for way in range(2):
                base = own(-(step + 2) if way == 0 else step + 2)
                lane = way * half + sub * sub_rows
                r_copy(step, way, sub).wait_recv()
                mine = part[pl.ds(pl.multiple_of(base + lane, sub_rows), sub_rows), :]
                total = (ring[step, way, sub].astype(F32) + mine.astype(F32)).astype(BF16)
                if step < n - 2:
                    ring[step, way, sub] = total
                    r_copy(step + 1, way, sub).start()
                else:
                    dh[lane : lane + sub_rows, :] = total

    def turn(device):
        turned[...] = h_all[:, pl.ds(pl.multiple_of(device * depth, depth), depth)].T

    def weight_part(j):
        return dot(turned[...], g_all[:, pl.ds(pl.multiple_of(j * columns, columns), columns)])

    def n_copy(o):
        return remote(near_out.at[o], near_in.at[o], n_send.at[o], n_recv.at[o], {"dp": mate})

    def f_copy(o, j):
        return remote(
            far_out.at[o - 1, j], far_in.at[o - 1, j], f_send.at[o - 1, j], f_recv.at[o - 1, j], {"dp": far(o)}
        )

    def near(o):
        turn(far(o) + 1 - 2 * core)

        @pl.loop(0, 3)
        def _(j):
            near_out[o, j] = weight_part(j).astype(BF16)

        n_copy(o).start()

    def chip_sum(o):
        turn(far(o))
        n_copy(o).wait_recv()
        if o:
            for j in range(3):
                far_out[o - 1, j] = (weight_part(j) + near_in[o, j].astype(F32)).astype(BF16)
                f_copy(o, j).start()
        else:
            for j, out in enumerate((dq, dk, dv)):
                out[...] = weight_part(j) + near_in[o, j].astype(F32)

    tasks = []
    for o in range(1, ny):
        tasks += [functools.partial(near, o), functools.partial(chip_sum, o)]
    tasks += [functools.partial(near, 0), functools.partial(chip_sum, 0)]

    compute(-1)
    for sub in range(SUBS):
        r_copy(0, 0, sub).start()
    compute(1)
    for sub in range(SUBS):
        r_copy(0, 1, sub).start()
    for step in range(n - 1):
        if tasks:
            tasks.pop(0)()
        compute(-(step + 2))
        compute(step + 2)
        process(step)
    while tasks:
        tasks.pop(0)()
    for j, out in enumerate((dq, dk, dv)):
        total = out[...]
        for o in range(1, ny):
            f_copy(o, j).wait_recv()
            total = total + far_in[o - 1, j].astype(F32)
        out[...] = total * (1.0 / m)
    for step in range(n - 1):
        for sub in range(SUBS):
            for way in range(2):
                r_copy(step, way, sub).wait_send()
    for o in range(ny):
        n_copy(o).wait_send()
        if o:
            for j in range(3):
                f_copy(o, j).wait_send()


def scatter(n, m, h_all, w_all, g_all):
    length, width = h_all.shape
    rows = length // n
    depth = width // m
    columns = w_all.shape[1] // 3
    ny = m // 2
    vmem = pl.BlockSpec(memory_space=pltpu.VMEM)
    dma = pltpu.SemaphoreType.DMA
    sub_rows = rows // 2 // SUBS
    return pl.pallas_call(
        functools.partial(scatter_kernel, n, m),
        out_shape=(jax.ShapeDtypeStruct((rows, width), BF16),)
        + (jax.ShapeDtypeStruct((depth, columns), F32),) * 3,
        in_specs=[vmem] * 3,
        out_specs=(vmem,) * 4,
        scratch_shapes=[
            pltpu.VMEM((length, width), BF16),
            pltpu.VMEM((n - 1, 2, SUBS, sub_rows, width), BF16),
            pltpu.VMEM((depth, length), BF16),
            pltpu.VMEM((ny, 3, depth, columns), BF16),
            pltpu.VMEM((ny, 3, depth, columns), BF16),
            pltpu.VMEM((ny - 1, 3, depth, columns), BF16),
            pltpu.VMEM((ny - 1, 3, depth, columns), BF16),
            dma((n - 1, 2, SUBS)),
            dma((n - 1, 2, SUBS)),
            dma((ny,)),
            dma((ny,)),
            dma((ny - 1, 3)),
            dma((ny - 1, 3)),
        ],
        compiler_params=pltpu.CompilerParams(
            collective_id=1, has_side_effects=True, vmem_limit_bytes=VMEM_LIMIT
        ),
        name="scatter_all",
    )(h_all, w_all, g_all)


def body(n, m, hidden_in, mix_cotangent, query_weight, key_weight, value_weight, decay_log):
    h_all, c_all, w_all = gather(
        n, m, hidden_in[0], mix_cotangent[0], query_weight, key_weight, value_weight
    )
    g_all = mixer(decay_log, h_all, c_all, w_all)
    dh, dq, dk, dv = scatter(n, m, h_all, w_all, g_all)
    return dh[None], dq, dk, dv


def solution(mesh):
    placed = (
        P("dp", "sp", None),
        P("dp", "sp", None),
        P("dp", "sp"),
        P("dp", "sp"),
        P("dp", "sp"),
        P("sp"),
    )
    return jax.shard_map(
        functools.partial(body, mesh.shape["sp"], mesh.shape["dp"]),
        mesh=mesh,
        in_specs=placed,
        out_specs=(P("dp", "sp", None), P("dp", "sp"), P("dp", "sp"), P("dp", "sp")),
        check_vma=False,
    )
```

```python
import functools

import jax
import jax.numpy as jnp
from jax import lax
from jax.experimental import pallas as pl
from jax.experimental.pallas import tpu as pltpu
from jax.sharding import PartitionSpec as P

BLOCK = 128
SUBS = 2
F32 = jnp.float32
BF16 = jnp.bfloat16
MESH = pl.DeviceIdType.MESH
NT = (((1,), (1,)), ((), ()))
TN = (((0,), (0,)), ((), ()))
VMEM_LIMIT = 56 * 1024 * 1024


def dot(a, b, dims=(((1,), (0,)), ((), ()))):
    return lax.dot_general(a, b, dims, preferred_element_type=F32)


def remote(src, dst, send, recv, where):
    return pltpu.make_async_remote_copy(
        src_ref=src, dst_ref=dst, send_sem=send, recv_sem=recv, device_id=where, device_id_type=MESH
    )


def greet(targets):
    barrier = pltpu.get_barrier_semaphore()
    for where in targets:
        pl.semaphore_signal(barrier, inc=1, device_id=where, device_id_type=MESH)
    pl.semaphore_wait(barrier, len(targets))


def gather_phase(
    n, m, project, h_in, c_in, wq, wk, wv, h_all, c_all, w_all,
    h_recv, h_line, h_side, c_send, c_recv, w_far, w_near, w_recv,
):
    s = lax.axis_index("sp")
    d = lax.axis_index("dp")
    z, x = s // 2, s % 2
    y, core = d // 2, d % 2
    nz, ny = n // 2, m // 2
    rows = h_in.shape[0]
    sub_rows = rows // SUBS
    depth, columns = wq.shape
    side = s + 1 - 2 * x
    mate = d + 1 - 2 * core

    def far(o):
        return ((y + o) % ny) * 2 + core

    greet(
        [{"sp": (s + k) % n} for k in range(1, n)]
        + [{"dp": mate}]
        + [{"dp": far(o)} for o in range(1, ny)]
    )

    def h_copy(src_z, src_x, sub, dest, send, own=False):
        block = src_z * 2 + src_x
        place = pl.ds(pl.multiple_of(block * rows + sub * sub_rows, sub_rows), sub_rows)
        src = h_in.at[pl.ds(sub * sub_rows, sub_rows)] if own else h_all.at[place]
        return remote(src, h_all.at[place], send, h_recv.at[block, sub], {"sp": dest})

    def w_copy(src_d, j, dest, send, own=False):
        place = w_all.at[
            pl.ds(pl.multiple_of(src_d * depth, depth), depth), pl.ds(j * columns, columns)
        ]
        return remote((wq, wk, wv)[j] if own else place, place, send, w_recv.at[src_d, j], {"dp": dest})

    def c_copy(k):
        to = (s + k) % n
        return remote(
            c_in.at[:, pl.ds(pl.multiple_of(to * columns, columns), columns)],
            c_all.at[pl.ds(pl.multiple_of(s * rows, rows), rows)],
            c_send.at[k - 1],
            c_recv.at[k - 1],
            {"sp": to},
        )

    def line(k, sub, up, own):
        source = (z - k) if up else (z + k)
        dest = (s + 2) if up else (s - 2)
        return h_copy(source, x, sub, dest, h_line.at[k, sub, int(up)], own)

    def goes(k, up):
        if up:
            return jnp.logical_and(z - k >= 0, z + 1 < nz)
        return jnp.logical_and(z + k < nz, z >= 1)

    def arrives(k, up):
        return (z - k >= 0) if up else (z + k < nz)

    for sub in range(SUBS):
        for up in (True, False):

            @pl.when(goes(0, up))
            def _():
                line(0, sub, up, True).start()

        h_copy(z, x, sub, side, h_side.at[0, sub, 0], True).start()
    for j in range(3):
        for o in range(1, ny):
            w_copy(d, j, far(o), w_far.at[o, j], True).start()
        w_copy(d, j, mate, w_near.at[0, j], True).start()

    h_all[pl.ds(pl.multiple_of(s * rows, rows), rows), :] = h_in[...]
    c_all[pl.ds(pl.multiple_of(s * rows, rows), rows), :] = c_in[
        :, pl.ds(pl.multiple_of(s * columns, columns), columns)
    ]
    for j, w in enumerate((wq, wk, wv)):
        w_all[pl.ds(pl.multiple_of(d * depth, depth), depth), j * columns : (j + 1) * columns] = w[...]

    def pass_weights(j):
        for o in range(1, ny):
            w_copy(far(o), j, mate, w_near.at[o, j]).wait_recv()
            w_copy(far(o), j, mate, w_near.at[o, j]).start()

    def send_cotangent():
        for hop in range(1, n):
            c_copy(hop).start()

    if nz < 2:
        send_cotangent()
    passed = 0
    for k in range(1, nz):
        for sub in range(SUBS):
            for up in (True, False):

                @pl.when(arrives(k, up))
                def _():
                    source = (z - k) if up else (z + k)
                    h_copy(source, x, sub, side, h_side.at[k, sub, int(up)]).wait_recv()
                    h_copy(source, x, sub, side, h_side.at[k, sub, int(up)]).start()

                @pl.when(goes(k, up))
                def _():
                    line(k, sub, up, False).start()

        if k == 1:
            send_cotangent()
        if passed < 3:
            pass_weights(passed)
            passed += 1
    for j in range(passed, 3):
        pass_weights(j)

    for j in range(3):
        w_copy(mate, j, mate, w_near.at[0, j]).wait_recv()
        for o in range(1, ny):
            other = far(o) + 1 - 2 * core
            w_copy(other, j, mate, w_near.at[o, j]).wait_recv()

    @pl.loop(0, nz)
    def _(zz):
        project(zz * 2 + x)

    turn = 1 - 2 * (z // ((nz + 1) // 2))

    @pl.loop(0, nz)
    def _(k):
        zz = (z + turn * k + nz) % nz
        for sub in range(SUBS):
            h_copy(zz, 1 - x, sub, side, h_side.at[0, sub, 0]).wait_recv()
        project(zz * 2 + 1 - x)

    for k in range(1, n):
        c_copy(k).wait_recv()
    def drain():
        for k in range(1, n):
            c_copy(k).wait_send()
        for j in range(3):
            for o in range(ny):
                w_copy(d, j, mate, w_near.at[o, j]).wait_send()
                if o:
                    w_copy(d, j, far(o), w_far.at[o, j]).wait_send()
        for sub in range(SUBS):
            h_copy(z, x, sub, side, h_side.at[0, sub, 0]).wait_send()
            for up in (True, False):
                for k in range(nz):

                    @pl.when(goes(k, up))
                    def _():
                        line(k, sub, up, False).wait_send()

                    if k:

                        @pl.when(arrives(k, up))
                        def _():
                            h_copy(z, x, sub, side, h_side.at[k, sub, int(up)]).wait_send()

    return drain


def project_block(h_all, w_all, p_all, rows, columns, scale, block):
    at = pl.ds(pl.multiple_of(block * rows, rows), rows)
    for j in range(3):
        value = dot(h_all[at, :], w_all[:, j * columns : (j + 1) * columns]).astype(BF16)
        if j == 1:
            value = (value.astype(F32) * scale).astype(BF16)
        p_all[at, j * columns : (j + 1) * columns] = value


def mixer_phase(heads, rate, c_all, p_all, g_all, state, back):
    length, columns = c_all.shape
    dim = columns // heads
    blocks = length // BLOCK
    scale = dim ** (-0.5)
    row = lax.broadcasted_iota(jnp.int32, (BLOCK, BLOCK), 0).astype(F32)
    col = lax.broadcasted_iota(jnp.int32, (BLOCK, BLOCK), 1).astype(F32)
    place = lax.broadcasted_iota(jnp.int32, (BLOCK, dim), 0).astype(F32)
    spread = row - col
    state[...] = jnp.zeros_like(state)
    back[...] = jnp.zeros_like(back)

    @pl.loop(0, blocks)
    def _(i):
        for h in range(heads):
            g = rate[h]
            inner = jnp.where(spread >= 0, jnp.exp(g * jnp.maximum(spread, 0.0)), 0.0)
            inner_t = jnp.where(spread <= 0, jnp.exp(g * jnp.maximum(-spread, 0.0)), 0.0)
            query_decay = jnp.exp(g * (place + 1.0))
            key_decay = jnp.exp(g * (BLOCK - 1.0 - place))
            block_decay = jnp.exp(jnp.full((1, dim), g * BLOCK, F32))
            parts = [slice(j * columns + h * dim, j * columns + (h + 1) * dim) for j in range(3)]

            at = pl.ds(pl.multiple_of(i * BLOCK, BLOCK), BLOCK)
            k, v = p_all[at, parts[1]], p_all[at, parts[2]]
            c = c_all[at, parts[0]]
            mixed = (dot(c, v, NT) * inner).astype(BF16)
            held = state[h]
            grad_q = dot(mixed, k) + dot(c, held.astype(BF16), NT) * query_decay
            weighted = (k.astype(F32) * key_decay).astype(BF16)
            state[h] = held * block_decay + dot(weighted, v, TN)
            g_all[at, parts[0]] = grad_q.astype(BF16)

            at = pl.ds(pl.multiple_of((blocks - 1 - i) * BLOCK, BLOCK), BLOCK)
            q, k, v = (p_all[at, part] for part in parts)
            c = c_all[at, parts[0]]
            mixed_t = (dot(v, c, NT) * inner_t).astype(BF16)
            scores_t = (dot(k, q, NT) * inner_t).astype(BF16)
            held = back[h]
            held_bf = held.astype(BF16)
            grad_v = dot(scores_t, c) + dot(k, held_bf) * key_decay
            grad_k = (dot(mixed_t, q) + dot(v, held_bf, NT) * key_decay) * scale
            weighted = (q.astype(F32) * query_decay).astype(BF16)
            back[h] = held * block_decay + dot(weighted, c, TN)
            g_all[at, parts[1]] = grad_k.astype(BF16)
            g_all[at, parts[2]] = grad_v.astype(BF16)


def scatter_phase(
    n, m, h_all, w_all, g_all, dh, dq, dk, dv,
    part, ring, turned, near_out, near_in, far_out, far_in,
    r_send, r_recv, n_send, n_recv, f_send, f_recv,
):
    s = lax.axis_index("sp")
    d = lax.axis_index("dp")
    z, x = s // 2, s % 2
    y, core = d // 2, d % 2
    nz, ny = n // 2, m // 2
    rows, width = dh.shape
    depth, columns = dq.shape
    half = rows // 2
    sub_rows = half // SUBS
    mate = d + 1 - 2 * core
    me = x * (n - 1 - z) + (1 - x) * z

    def at_ring(p):
        p = (p + 2 * n) % n
        hi = p // nz
        return (hi * (n - 1 - p) + (1 - hi) * p) * 2 + hi

    def far(o):
        return ((y + o) % ny) * 2 + core

    right, left = at_ring(me + 1), at_ring(me - 1)

    def own(offset):
        return pl.multiple_of(at_ring(me + offset) * rows, rows)

    ready = set()

    def compute(*offsets):
        todo = []
        for offset in offsets:
            if offset % n not in ready:
                ready.add(offset % n)
                todo.append(own(offset))
        if not todo:
            return
        chunk = width // 4

        @pl.loop(0, 4)
        def _(i):
            at = pl.ds(pl.multiple_of(i * chunk, chunk), chunk)
            lhs = jnp.concatenate([g_all[pl.ds(base, rows), :] for base in todo], axis=0)
            value = dot(lhs, w_all[at, :], NT).astype(BF16)
            for spot, base in enumerate(todo):
                part[pl.ds(base, rows), at] = value[spot * rows : (spot + 1) * rows]

    def r_copy(step, way, sub):
        lane = (slice(0, half), slice(half, rows))[way].start + sub * sub_rows
        if step == 0:
            base = own(-1 if way == 0 else 1)
            src = part.at[pl.ds(pl.multiple_of(base + lane, sub_rows), sub_rows)]
        else:
            src = ring.at[step - 1, way, sub]
        return remote(
            src,
            ring.at[step, way, sub],
            r_send.at[step, way, sub],
            r_recv.at[step, way, sub],
            {"sp": right if way == 0 else left},
        )

    def process(step):
        for sub in range(SUBS):
            for way in range(2):
                base = own(-(step + 2) if way == 0 else step + 2)
                lane = way * half + sub * sub_rows
                r_copy(step, way, sub).wait_recv()
                mine = part[pl.ds(pl.multiple_of(base + lane, sub_rows), sub_rows), :]
                total = (ring[step, way, sub].astype(F32) + mine.astype(F32)).astype(BF16)
                if step < n - 2:
                    ring[step, way, sub] = total
                    r_copy(step + 1, way, sub).start()
                else:
                    dh[lane : lane + sub_rows, :] = total

    def turn(device):
        turned[...] = h_all[:, pl.ds(pl.multiple_of(device * depth, depth), depth)].T

    def weight_part(j):
        return dot(turned[...], g_all[:, pl.ds(pl.multiple_of(j * columns, columns), columns)])

    def n_copy(o):
        return remote(near_out.at[o], near_in.at[o], n_send.at[o], n_recv.at[o], {"dp": mate})

    def f_copy(o, j):
        return remote(
            far_out.at[o - 1, j], far_in.at[o - 1, j], f_send.at[o - 1, j], f_recv.at[o - 1, j], {"dp": far(o)}
        )

    def near(o):
        turn(far(o) + 1 - 2 * core)

        @pl.loop(0, 3)
        def _(j):
            near_out[o, j] = weight_part(j).astype(BF16)

        n_copy(o).start()

    def chip_sum(o):
        turn(far(o))
        n_copy(o).wait_recv()
        if o:
            for j in range(3):
                far_out[o - 1, j] = (weight_part(j) + near_in[o, j].astype(F32)).astype(BF16)
                f_copy(o, j).start()
        else:
            for j, out in enumerate((dq, dk, dv)):
                out[...] = weight_part(j) + near_in[o, j].astype(F32)

    tasks = []
    for o in range(1, ny):
        tasks += [functools.partial(near, o), functools.partial(chip_sum, o)]
    tasks += [functools.partial(near, 0), functools.partial(chip_sum, 0)]

    compute(-1, 1)
    for sub in range(SUBS):
        for way in range(2):
            r_copy(0, way, sub).start()
    for step in range(n - 1):
        early = step % 2 == 0
        if early and tasks:
            tasks.pop(0)()
        compute(-(step + 2), step + 2)
        process(step)
        if not early and tasks:
            tasks.pop(0)()
        if step == 0 and tasks:
            tasks.pop(0)()
        if step + 3 == n // 2:
            compute(n // 2, 0)
    while tasks:
        tasks.pop(0)()
    for j, out in enumerate((dq, dk, dv)):
        total = out[...]
        for o in range(1, ny):
            f_copy(o, j).wait_recv()
            total = total + far_in[o - 1, j].astype(F32)
        out[...] = total * (1.0 / m)
    for step in range(n - 1):
        for sub in range(SUBS):
            for way in range(2):
                r_copy(step, way, sub).wait_send()
    for o in range(ny):
        n_copy(o).wait_send()
        if o:
            for j in range(3):
                f_copy(o, j).wait_send()


def whole_kernel(n, m, heads, rate, h_in, c_in, wq, wk, wv, dh, dq, dk, dv, *scratch):
    h_all, c_all, w_all, p_all, g_all, state, back = scratch[:7]
    gather_sems, rest = scratch[7:15], scratch[15:]
    columns = wq.shape[1]
    project = functools.partial(
        project_block, h_all, w_all, p_all, h_in.shape[0], columns, (columns // heads) ** (-0.5)
    )
    drain = gather_phase(
        n, m, project, h_in, c_in, wq, wk, wv, h_all, c_all, w_all, *gather_sems
    )
    mixer_phase(heads, rate, c_all, p_all, g_all, state, back)
    scatter_phase(n, m, h_all, w_all, g_all, dh, dq, dk, dv, *rest)
    drain()


def whole(n, m, rate, h, c, wq, wk, wv):
    rows, width = h.shape
    depth, columns = wq.shape
    heads = rate.shape[0]
    dim = columns // heads
    length = rows * n
    ny = m // 2
    vmem = pl.BlockSpec(memory_space=pltpu.VMEM)
    dma = pltpu.SemaphoreType.DMA
    sub_rows = rows // 2 // SUBS
    return pl.pallas_call(
        functools.partial(whole_kernel, n, m, heads),
        out_shape=(jax.ShapeDtypeStruct((rows, width), BF16),)
        + (jax.ShapeDtypeStruct((depth, columns), F32),) * 3,
        in_specs=[pl.BlockSpec(memory_space=pltpu.SMEM)] + [vmem] * 5,
        out_specs=(vmem,) * 4,
        scratch_shapes=[
            pltpu.VMEM((length, width), BF16),
            pltpu.VMEM((length, columns), BF16),
            pltpu.VMEM((depth * m, 3 * columns), BF16),
            pltpu.VMEM((length, 3 * columns), BF16),
            pltpu.VMEM((length, 3 * columns), BF16),
            pltpu.VMEM((heads, dim, dim), F32),
            pltpu.VMEM((heads, dim, dim), F32),
            dma((n, SUBS)),
            dma((n // 2, SUBS, 2)),
            dma((n // 2, SUBS, 2)),
            dma((n - 1,)),
            dma((n - 1,)),
            dma((ny, 3)),
            dma((ny, 3)),
            dma((m, 3)),
            pltpu.VMEM((length, width), BF16),
            pltpu.VMEM((n - 1, 2, SUBS, sub_rows, width), BF16),
            pltpu.VMEM((depth, length), BF16),
            pltpu.VMEM((ny, 3, depth, columns), BF16),
            pltpu.VMEM((ny, 3, depth, columns), BF16),
            pltpu.VMEM((ny - 1, 3, depth, columns), BF16),
            pltpu.VMEM((ny - 1, 3, depth, columns), BF16),
            dma((n - 1, 2, SUBS)),
            dma((n - 1, 2, SUBS)),
            dma((ny,)),
            dma((ny,)),
            dma((ny - 1, 3)),
            dma((ny - 1, 3)),
        ],
        compiler_params=pltpu.CompilerParams(
            collective_id=0, has_side_effects=True, vmem_limit_bytes=VMEM_LIMIT
        ),
        name="whole",
    )(rate, h, c, wq, wk, wv)


def finish_kernel(count, *refs):
    ins, outs, held = refs[:count], refs[count : 2 * count], refs[2 * count : 3 * count]
    sems = refs[3 * count]
    moves = []
    for i in range(count):
        piece = ins[i].shape[0] // 2
        for half in range(2):
            at = pl.ds(half * piece, piece)
            moves.append(
                (
                    pltpu.make_async_copy(ins[i].at[at], held[i].at[at], sems.at[0, i, half]),
                    pltpu.make_async_copy(held[i].at[at], outs[i].at[at], sems.at[1, i, half]),
                )
            )
    for fetch, _ in moves:
        fetch.start()
    for fetch, put in moves:
        fetch.wait()
        put.start()
    for _, put in moves:
        put.wait()


def finish(*arrays):
    spec = pl.BlockSpec(memory_space=pl.ANY)
    count = len(arrays)
    return pl.pallas_call(
        functools.partial(finish_kernel, count),
        out_shape=tuple(jax.ShapeDtypeStruct(a.shape, a.dtype) for a in arrays),
        in_specs=[spec] * count,
        out_specs=(spec,) * count,
        scratch_shapes=[pltpu.VMEM(a.shape, a.dtype) for a in arrays]
        + [pltpu.SemaphoreType.DMA((2, count, 2))],
        name="finish",
    )(*arrays)


def body(n, m, hidden_in, mix_cotangent, query_weight, key_weight, value_weight, decay_log):
    dh, dq, dk, dv = finish(
        *whole(
            n, m, decay_log, hidden_in[0], mix_cotangent[0], query_weight, key_weight, value_weight
        )
    )
    return dh[None], dq, dk, dv


def solution(mesh):
    placed = (
        P("dp", "sp", None),
        P("dp", "sp", None),
        P("dp", "sp"),
        P("dp", "sp"),
        P("dp", "sp"),
        P("sp"),
    )
    return jax.shard_map(
        functools.partial(body, mesh.shape["sp"], mesh.shape["dp"]),
        mesh=mesh,
        in_specs=placed,
        out_specs=(P("dp", "sp", None), P("dp", "sp"), P("dp", "sp"), P("dp", "sp")),
        check_vma=False,
    )
```

```python
import functools

import jax
import jax.numpy as jnp
from jax import lax
from jax.experimental import pallas as pl
from jax.experimental.pallas import tpu as pltpu
from jax.sharding import PartitionSpec as P

BLOCK = 128
SUBS = 2
F32 = jnp.float32
BF16 = jnp.bfloat16
MESH = pl.DeviceIdType.MESH
NT = (((1,), (1,)), ((), ()))
TN = (((0,), (0,)), ((), ()))
VMEM_LIMIT = 52 * 1024 * 1024


def dot(a, b, dims=(((1,), (0,)), ((), ()))):
    return lax.dot_general(a, b, dims, preferred_element_type=F32)


def remote(src, dst, send, recv, where):
    return pltpu.make_async_remote_copy(
        src_ref=src, dst_ref=dst, send_sem=send, recv_sem=recv, device_id=where, device_id_type=MESH
    )


def greet(targets):
    barrier = pltpu.get_barrier_semaphore()
    for where in targets:
        pl.semaphore_signal(barrier, inc=1, device_id=where, device_id_type=MESH)
    pl.semaphore_wait(barrier, len(targets))


def gather_phase(
    n, m, project, h_in, c_in, wq, wk, wv, h_all, c_all, w_all,
    h_recv, h_line, h_side, c_send, c_recv, w_far, w_near, w_recv,
):
    s = lax.axis_index("sp")
    d = lax.axis_index("dp")
    z, x = s // 2, s % 2
    y, core = d // 2, d % 2
    nz, ny = n // 2, m // 2
    rows = h_in.shape[0]
    sub_rows = rows // SUBS
    depth, columns = wq.shape
    side = s + 1 - 2 * x
    mate = d + 1 - 2 * core

    def far(o):
        return ((y + o) % ny) * 2 + core

    greet(
        [{"sp": (s + k) % n} for k in range(1, n)]
        + [{"dp": mate}]
        + [{"dp": far(o)} for o in range(1, ny)]
    )

    def h_copy(src_z, src_x, sub, dest, send, own=False):
        block = src_z * 2 + src_x
        place = pl.ds(pl.multiple_of(block * rows + sub * sub_rows, sub_rows), sub_rows)
        src = h_in.at[pl.ds(sub * sub_rows, sub_rows)] if own else h_all.at[place]
        return remote(src, h_all.at[place], send, h_recv.at[block, sub], {"sp": dest})

    def w_copy(src_d, j, dest, send, own=False):
        place = w_all.at[
            pl.ds(pl.multiple_of(src_d * depth, depth), depth), pl.ds(j * columns, columns)
        ]
        return remote((wq, wk, wv)[j] if own else place, place, send, w_recv.at[src_d, j], {"dp": dest})

    def c_copy(k):
        to = (s + k) % n
        return remote(
            c_in.at[:, pl.ds(pl.multiple_of(to * columns, columns), columns)],
            c_all.at[pl.ds(pl.multiple_of(s * rows, rows), rows)],
            c_send.at[k - 1],
            c_recv.at[k - 1],
            {"sp": to},
        )

    def line(k, sub, up, own):
        source = (z - k) if up else (z + k)
        dest = (s + 2) if up else (s - 2)
        return h_copy(source, x, sub, dest, h_line.at[k, sub, int(up)], own)

    def goes(k, up):
        if up:
            return jnp.logical_and(z - k >= 0, z + 1 < nz)
        return jnp.logical_and(z + k < nz, z >= 1)

    def arrives(k, up):
        return (z - k >= 0) if up else (z + k < nz)

    for sub in range(SUBS):
        for up in (True, False):

            @pl.when(goes(0, up))
            def _():
                line(0, sub, up, True).start()

        h_copy(z, x, sub, side, h_side.at[0, sub, 0], True).start()
    for j in range(3):
        for o in range(1, ny):
            w_copy(d, j, far(o), w_far.at[o, j], True).start()
        w_copy(d, j, mate, w_near.at[0, j], True).start()

    h_all[pl.ds(pl.multiple_of(s * rows, rows), rows), :] = h_in[...]
    c_all[pl.ds(pl.multiple_of(s * rows, rows), rows), :] = c_in[
        :, pl.ds(pl.multiple_of(s * columns, columns), columns)
    ]
    for j, w in enumerate((wq, wk, wv)):
        w_all[pl.ds(pl.multiple_of(d * depth, depth), depth), j * columns : (j + 1) * columns] = w[...]

    def pass_weights(j):
        for o in range(1, ny):
            w_copy(far(o), j, mate, w_near.at[o, j]).wait_recv()
            w_copy(far(o), j, mate, w_near.at[o, j]).start()

    def send_cotangent():
        for hop in range(1, n):
            c_copy(hop).start()

    passed = 0
    for k in range(1, nz):
        for sub in range(SUBS):
            for up in (True, False):

                @pl.when(arrives(k, up))
                def _():
                    source = (z - k) if up else (z + k)
                    h_copy(source, x, sub, side, h_side.at[k, sub, int(up)]).wait_recv()
                    h_copy(source, x, sub, side, h_side.at[k, sub, int(up)]).start()

                @pl.when(goes(k, up))
                def _():
                    line(k, sub, up, False).start()

    send_cotangent()
    for j in range(passed, 3):
        pass_weights(j)

    for j in range(3):
        w_copy(mate, j, mate, w_near.at[0, j]).wait_recv()
        for o in range(1, ny):
            other = far(o) + 1 - 2 * core
            w_copy(other, j, mate, w_near.at[o, j]).wait_recv()

    @pl.loop(0, nz)
    def _(zz):
        project(zz * 2 + x)

    turn = 1 - 2 * (z // ((nz + 1) // 2))

    @pl.loop(0, nz)
    def _(k):
        zz = (z + turn * k + nz) % nz
        for sub in range(SUBS):
            h_copy(zz, 1 - x, sub, side, h_side.at[0, sub, 0]).wait_recv()
        project(zz * 2 + 1 - x)

    for k in range(1, n):
        c_copy(k).wait_recv()
    def drain():
        for k in range(1, n):
            c_copy(k).wait_send()
        for j in range(3):
            for o in range(ny):
                w_copy(d, j, mate, w_near.at[o, j]).wait_send()
                if o:
                    w_copy(d, j, far(o), w_far.at[o, j]).wait_send()
        for sub in range(SUBS):
            h_copy(z, x, sub, side, h_side.at[0, sub, 0]).wait_send()
            for up in (True, False):
                for k in range(nz):

                    @pl.when(goes(k, up))
                    def _():
                        line(k, sub, up, False).wait_send()

                    if k:

                        @pl.when(arrives(k, up))
                        def _():
                            h_copy(z, x, sub, side, h_side.at[k, sub, int(up)]).wait_send()

    return drain


def project_block(h_all, w_all, p_all, rows, columns, scale, block):
    at = pl.ds(pl.multiple_of(block * rows, rows), rows)
    for j in range(3):
        value = dot(h_all[at, :], w_all[:, j * columns : (j + 1) * columns]).astype(BF16)
        if j == 1:
            value = (value.astype(F32) * scale).astype(BF16)
        p_all[at, j * columns : (j + 1) * columns] = value


def mixer_phase(heads, rate, c_all, p_all, g_all, state, back):
    length, columns = c_all.shape
    dim = columns // heads
    blocks = length // BLOCK
    scale = dim ** (-0.5)
    row = lax.broadcasted_iota(jnp.int32, (BLOCK, BLOCK), 0).astype(F32)
    col = lax.broadcasted_iota(jnp.int32, (BLOCK, BLOCK), 1).astype(F32)
    place = lax.broadcasted_iota(jnp.int32, (BLOCK, dim), 0).astype(F32)
    spread = row - col
    state[...] = jnp.zeros_like(state)
    back[...] = jnp.zeros_like(back)

    @pl.loop(0, blocks)
    def _(i):
        for h in range(heads):
            g = rate[h]
            inner = jnp.where(spread >= 0, jnp.exp(g * jnp.maximum(spread, 0.0)), 0.0)
            inner_t = jnp.where(spread <= 0, jnp.exp(g * jnp.maximum(-spread, 0.0)), 0.0)
            query_decay = jnp.exp(g * (place + 1.0))
            key_decay = jnp.exp(g * (BLOCK - 1.0 - place))
            block_decay = jnp.exp(jnp.full((1, dim), g * BLOCK, F32))
            parts = [slice(j * columns + h * dim, j * columns + (h + 1) * dim) for j in range(3)]

            at = pl.ds(pl.multiple_of(i * BLOCK, BLOCK), BLOCK)
            k, v = p_all[at, parts[1]], p_all[at, parts[2]]
            c = c_all[at, parts[0]]
            mixed = (dot(c, v, NT) * inner).astype(BF16)
            held = state[h]
            grad_q = dot(mixed, k) + dot(c, held.astype(BF16), NT) * query_decay
            weighted = (k.astype(F32) * key_decay).astype(BF16)
            state[h] = held * block_decay + dot(weighted, v, TN)
            g_all[at, parts[0]] = grad_q.astype(BF16)

            at = pl.ds(pl.multiple_of((blocks - 1 - i) * BLOCK, BLOCK), BLOCK)
            q, k, v = (p_all[at, part] for part in parts)
            c = c_all[at, parts[0]]
            mixed_t = (dot(v, c, NT) * inner_t).astype(BF16)
            scores_t = (dot(k, q, NT) * inner_t).astype(BF16)
            held = back[h]
            held_bf = held.astype(BF16)
            grad_v = dot(scores_t, c) + dot(k, held_bf) * key_decay
            grad_k = (dot(mixed_t, q) + dot(v, held_bf, NT) * key_decay) * scale
            weighted = (q.astype(F32) * query_decay).astype(BF16)
            back[h] = held * block_decay + dot(weighted, c, TN)
            g_all[at, parts[1]] = grad_k.astype(BF16)
            g_all[at, parts[2]] = grad_v.astype(BF16)


def scatter_phase(
    n, m, h_all, w_all, g_all, dh, dq, dk, dv,
    part, ring, turned, near_out, near_in, far_out, far_in,
    r_send, r_recv, n_send, n_recv, f_send, f_recv,
):
    s = lax.axis_index("sp")
    d = lax.axis_index("dp")
    z, x = s // 2, s % 2
    y, core = d // 2, d % 2
    nz, ny = n // 2, m // 2
    rows, width = dh.shape
    depth, columns = dq.shape
    half = rows // 2
    sub_rows = half // SUBS
    mate = d + 1 - 2 * core
    me = x * (n - 1 - z) + (1 - x) * z

    def at_ring(p):
        p = (p + 2 * n) % n
        hi = p // nz
        return (hi * (n - 1 - p) + (1 - hi) * p) * 2 + hi

    def far(o):
        return ((y + o) % ny) * 2 + core

    right, left = at_ring(me + 1), at_ring(me - 1)

    def own(offset):
        return pl.multiple_of(at_ring(me + offset) * rows, rows)

    ready = set()

    def compute(*offsets):
        todo = []
        for offset in offsets:
            if offset % n not in ready:
                ready.add(offset % n)
                todo.append(own(offset))
        if not todo:
            return
        chunk = width // 4

        @pl.loop(0, 4)
        def _(i):
            at = pl.ds(pl.multiple_of(i * chunk, chunk), chunk)
            lhs = jnp.concatenate([g_all[pl.ds(base, rows), :] for base in todo], axis=0)
            value = dot(lhs, w_all[at, :], NT).astype(BF16)
            for spot, base in enumerate(todo):
                part[pl.ds(base, rows), at] = value[spot * rows : (spot + 1) * rows]

    def r_copy(step, way, sub):
        lane = (slice(0, half), slice(half, rows))[way].start + sub * sub_rows
        if step == 0:
            base = own(-1 if way == 0 else 1)
            src = part.at[pl.ds(pl.multiple_of(base + lane, sub_rows), sub_rows)]
        else:
            src = ring.at[step - 1, way, sub]
        return remote(
            src,
            ring.at[step, way, sub],
            r_send.at[step, way, sub],
            r_recv.at[step, way, sub],
            {"sp": right if way == 0 else left},
        )

    def process(step):
        for sub in range(SUBS):
            for way in range(2):
                base = own(-(step + 2) if way == 0 else step + 2)
                lane = way * half + sub * sub_rows
                r_copy(step, way, sub).wait_recv()
                mine = part[pl.ds(pl.multiple_of(base + lane, sub_rows), sub_rows), :]
                total = (ring[step, way, sub].astype(F32) + mine.astype(F32)).astype(BF16)
                if step < n - 2:
                    ring[step, way, sub] = total
                    r_copy(step + 1, way, sub).start()
                else:
                    dh[lane : lane + sub_rows, :] = total

    def turn(device):
        turned[...] = h_all[:, pl.ds(pl.multiple_of(device * depth, depth), depth)].T

    def weight_part(j):
        return dot(turned[...], g_all[:, pl.ds(pl.multiple_of(j * columns, columns), columns)])

    def n_copy(o):
        return remote(near_out.at[o], near_in.at[o], n_send.at[o], n_recv.at[o], {"dp": mate})

    def f_copy(o, j):
        return remote(
            far_out.at[o - 1, j], far_in.at[o - 1, j], f_send.at[o - 1, j], f_recv.at[o - 1, j], {"dp": far(o)}
        )

    def near(o):
        turn(far(o) + 1 - 2 * core)

        @pl.loop(0, 3)
        def _(j):
            near_out[o, j] = weight_part(j).astype(BF16)

        n_copy(o).start()

    def chip_sum(o):
        turn(far(o))
        n_copy(o).wait_recv()
        if o:
            for j in range(3):
                far_out[o - 1, j] = (weight_part(j) + near_in[o, j].astype(F32)).astype(BF16)
                f_copy(o, j).start()
        else:
            for j, out in enumerate((dq, dk, dv)):
                out[...] = weight_part(j) + near_in[o, j].astype(F32)

    tasks = []
    for o in range(1, ny):
        tasks += [functools.partial(near, o), functools.partial(chip_sum, o)]
    tasks += [functools.partial(near, 0), functools.partial(chip_sum, 0)]

    compute(-1, 1)
    for sub in range(SUBS):
        for way in range(2):
            r_copy(0, way, sub).start()
    for step in range(n - 1):
        early = step % 2 == 0
        if early and tasks:
            tasks.pop(0)()
        compute(-(step + 2), step + 2)
        process(step)
        if not early and tasks:
            tasks.pop(0)()
        if step == 0 and tasks:
            tasks.pop(0)()
        if step + 3 == n // 2:
            compute(n // 2, 0)
    while tasks:
        tasks.pop(0)()
    for j, out in enumerate((dq, dk, dv)):
        total = out[...]
        for o in range(1, ny):
            f_copy(o, j).wait_recv()
            total = total + far_in[o - 1, j].astype(F32)
        out[...] = total * (1.0 / m)
    for step in range(n - 1):
        for sub in range(SUBS):
            for way in range(2):
                r_copy(step, way, sub).wait_send()
    for o in range(ny):
        n_copy(o).wait_send()
        if o:
            for j in range(3):
                f_copy(o, j).wait_send()


def whole_kernel(n, m, heads, rate, h_in, c_in, wq, wk, wv, dh, dq, dk, dv, *scratch):
    h_all, c_all, w_all, p_all, g_all, state, back = scratch[:7]
    gather_sems, rest = scratch[7:15], scratch[15:]
    columns = wq.shape[1]
    project = functools.partial(
        project_block, h_all, w_all, p_all, h_in.shape[0], columns, (columns // heads) ** (-0.5)
    )
    drain = gather_phase(
        n, m, project, h_in, c_in, wq, wk, wv, h_all, c_all, w_all, *gather_sems
    )
    mixer_phase(heads, rate, c_all, p_all, g_all, state, back)
    scatter_phase(n, m, h_all, w_all, g_all, dh, dq, dk, dv, *rest)
    drain()


def whole(n, m, rate, h, c, wq, wk, wv):
    rows, width = h.shape
    depth, columns = wq.shape
    heads = rate.shape[0]
    dim = columns // heads
    length = rows * n
    ny = m // 2
    vmem = pl.BlockSpec(memory_space=pltpu.VMEM)
    dma = pltpu.SemaphoreType.DMA
    sub_rows = rows // 2 // SUBS
    return pl.pallas_call(
        functools.partial(whole_kernel, n, m, heads),
        out_shape=(pltpu.VMEM((rows, width), BF16),)
        + (pltpu.VMEM((depth, columns), F32),) * 3,
        in_specs=[pl.BlockSpec(memory_space=pltpu.SMEM)] + [vmem] * 5,
        out_specs=(vmem,) * 4,
        scratch_shapes=[
            pltpu.VMEM((length, width), BF16),
            pltpu.VMEM((length, columns), BF16),
            pltpu.VMEM((depth * m, 3 * columns), BF16),
            pltpu.VMEM((length, 3 * columns), BF16),
            pltpu.VMEM((length, 3 * columns), BF16),
            pltpu.VMEM((heads, dim, dim), F32),
            pltpu.VMEM((heads, dim, dim), F32),
            dma((n, SUBS)),
            dma((n // 2, SUBS, 2)),
            dma((n // 2, SUBS, 2)),
            dma((n - 1,)),
            dma((n - 1,)),
            dma((ny, 3)),
            dma((ny, 3)),
            dma((m, 3)),
            pltpu.VMEM((length, width), BF16),
            pltpu.VMEM((n - 1, 2, SUBS, sub_rows, width), BF16),
            pltpu.VMEM((depth, length), BF16),
            pltpu.VMEM((ny, 3, depth, columns), BF16),
            pltpu.VMEM((ny, 3, depth, columns), BF16),
            pltpu.VMEM((ny - 1, 3, depth, columns), BF16),
            pltpu.VMEM((ny - 1, 3, depth, columns), BF16),
            dma((n - 1, 2, SUBS)),
            dma((n - 1, 2, SUBS)),
            dma((ny,)),
            dma((ny,)),
            dma((ny - 1, 3)),
            dma((ny - 1, 3)),
        ],
        compiler_params=pltpu.CompilerParams(
            collective_id=0, has_side_effects=True, vmem_limit_bytes=VMEM_LIMIT
        ),
        name="whole",
    )(rate, h, c, wq, wk, wv)


def finish_kernel(count, *refs):
    ins, outs, sems = refs[:count], refs[count : 2 * count], refs[2 * count]
    moves = [pltpu.make_async_copy(ins[i], outs[i], sems.at[i]) for i in range(count)]
    for move in moves:
        move.start()
    for move in moves:
        move.wait()


def finish(*arrays):
    count = len(arrays)
    return pl.pallas_call(
        functools.partial(finish_kernel, count),
        out_shape=tuple(jax.ShapeDtypeStruct(a.shape, a.dtype) for a in arrays),
        in_specs=[pl.BlockSpec(memory_space=pltpu.VMEM)] * count,
        out_specs=(pl.BlockSpec(memory_space=pl.ANY),) * count,
        scratch_shapes=[pltpu.SemaphoreType.DMA((count,))],
        compiler_params=pltpu.CompilerParams(vmem_limit_bytes=4 * 1024 * 1024),
        name="finish",
    )(*arrays)


def body(n, m, hidden_in, mix_cotangent, query_weight, key_weight, value_weight, decay_log):
    dh, dq, dk, dv = finish(
        *whole(
            n, m, decay_log, hidden_in[0], mix_cotangent[0], query_weight, key_weight, value_weight
        )
    )
    return dh[None], dq, dk, dv


def solution(mesh):
    placed = (
        P("dp", "sp", None),
        P("dp", "sp", None),
        P("dp", "sp"),
        P("dp", "sp"),
        P("dp", "sp"),
        P("sp"),
    )
    return jax.shard_map(
        functools.partial(body, mesh.shape["sp"], mesh.shape["dp"]),
        mesh=mesh,
        in_specs=placed,
        out_specs=(P("dp", "sp", None), P("dp", "sp"), P("dp", "sp"), P("dp", "sp")),
        check_vma=False,
    )
```
